32 devices in a mesh: sp: 4 (over z), fs: 4 (over y, x), tp: 2 (over core).
Axes of the slice: x: 2, y: 2, z: 4, core: 2. Of those that a mesh axis runs over, the one named last changes fastest.
Arguments:
- tokens: bfloat16 [4, 1024, 2048], P('fs', 'sp', 'tp'), may hold values from -6 to 6
- norm_gain: float32 [2048], replicated, may hold values from 0.1 to 1.9
- query_weight: bfloat16 [2048, 1024], P('fs', 'tp'), may hold values from -1 to 1
- key_weight: bfloat16 [2048, 1024], P('fs', 'tp'), may hold values from -4 to 4
- value_weight: bfloat16 [2048, 1024], P('fs', 'tp'), may hold values from -0.125 to 0.125
- state_query: bfloat16 [2048, 1024], P('fs', 'tp'), may hold values from -0.125 to 0.125
- state_key: bfloat16 [2048, 1024], P('fs', 'tp'), may hold values from -0.125 to 0.125
- state_value: bfloat16 [2048, 1024], P('fs', 'tp'), may hold values from -0.125 to 0.125
- map_lambda: float32 [8], P('tp'), may hold values from 0.3 to 0.8
- diff_gain: float32 [1024], P('tp'), may hold values from 0.1 to 1.9
- decay_rate: float32 [8], P('tp'), may hold values from 0 to 0.04
- state_gain: float32 [1024], P('tp'), may hold values from 0.1 to 1.9
- out_weight: bfloat16 [2048, 2048], replicated, may hold values from -0.125 to 0.125
Outputs:
- mixed: bfloat16 [4, 1024, 2048], P('fs', ('sp', 'tp'))
The draws below stay inside these ranges and needn't reach their ends.
All inputs are finite; a program needn't handle non-finite values.
Results may differ from the reference program's by a relative error of at most 0.015.
Values may be sent and summed in bfloat16 or wider, within the bound.
No kernel may reach another device: no remote copies, remote signals or barrier semaphores. Data moves between devices by JAX's collectives and lax.ppermute only.
A program may use at most 128 MiB of HBM per device.

```python
import math
import jax
import jax.numpy as jnp
from jax import lax

D = 2048
HD = 8
DK = 64
DV = 128
HR = 8
DR = 128
TOK_DEV = 256
LENGTH = 1024
SEQS = 4


def query_base(key):
    return jax.random.normal(jax.random.fold_in(key, 101), (D, HD * 2 * DK), jnp.float32) * (2.0 / D) ** 0.5


def draw_query_weight(key, part):
    return jnp.clip(query_base(key), -1.0, 1.0).astype(jnp.bfloat16)


def draw_key_weight(key, part):
    fresh = jax.random.normal(jax.random.fold_in(key, 202), (D, HD * 2 * DK), jnp.float32) * (2.0 / D) ** 0.5
    result = fresh
    return jnp.clip(result, -4.0, 4.0).astype(jnp.bfloat16)


def draw_decay_rate(key, part):
    pick = jax.random.uniform(jax.random.fold_in(key, 404), (HR,), jnp.float32)
    share = 0.5
    slow_rate = jnp.exp(jax.random.uniform(jax.random.fold_in(key, 505), (HR,), jnp.float32, math.log(0.1), math.log(2.0))) / LENGTH
    fast_rate = jnp.exp(jax.random.uniform(jax.random.fold_in(key, 606), (HR,), jnp.float32, math.log(0.01), math.log(0.033)))
    return jnp.where(pick < share, slow_rate, fast_rate)


def shard_levels(key, shape, pieces, smallest, high):
    level, own = 1.0, jax.random.fold_in(key, 6)
    for dim, blocks in pieces:
        steps = jnp.exp(jax.random.uniform(jax.random.fold_in(own, dim), (blocks,), jnp.float32, smallest / len(pieces), high / len(pieces)))
        level = level * jnp.repeat(steps, shape[dim] // blocks).reshape([-1 if axis == dim else 1 for axis in range(len(shape))])
    return level


def scatter_about(rng, dims, width, most, shards=(), held_as=jnp.bfloat16):
    drawn = width * jax.random.normal(rng, dims, jnp.float32)
    if shards:
        drawn = drawn * shard_levels(rng, dims, shards, -0.22, 0.18)
    return jnp.clip(drawn, -most, most).astype(held_as)


def setup_inputs(seed: int = 0) -> dict:
    key_list = jax.random.split(jax.random.key(seed), 14)
    return {
        "tokens": scatter_about(key_list[0], (SEQS, LENGTH, D), 1.0, 6.0, ((0, 4), (1, 4), (2, 2))),
        "norm_gain": jnp.clip(1.0 + 0.18 * jax.random.normal(key_list[1], (D,), jnp.float32), 0.1, 1.9),
        "query_weight": draw_query_weight(jax.random.fold_in(key_list[13], 71), 0),
        "key_weight": draw_key_weight(jax.random.fold_in(key_list[13], 71), 0),
        "value_weight": scatter_about(key_list[4], (D, HD * DV), D ** -0.5, 0.125, ((0, 4), (1, 2))),
        "state_query": scatter_about(key_list[5], (D, HR * DR), D ** -0.5, 0.125, ((0, 4), (1, 2))),
        "state_key": scatter_about(key_list[6], (D, HR * DR), D ** -0.5, 0.125, ((0, 4), (1, 2))),
        "state_value": scatter_about(key_list[7], (D, HR * DR), D ** -0.5, 0.125, ((0, 4), (1, 2))),
        "map_lambda": jnp.clip(0.3 + 0.5 * jax.random.uniform(key_list[8], (HD,), jnp.float32) ** shard_levels(key_list[8], (HD,), ((0, 2),), -0.2, 0.2), 0.3, 0.8),
        "diff_gain": jnp.clip(1.0 + 0.18 * jax.random.normal(key_list[9], (HD * DV,), jnp.float32), 0.1, 1.9),
        "decay_rate": draw_decay_rate(jax.random.fold_in(key_list[13], 71), 0),
        "state_gain": jnp.clip(1.0 + 0.18 * jax.random.normal(key_list[11], (HR * DR,), jnp.float32), 0.1, 1.9),
        "out_weight": scatter_about(key_list[12], (HD * DV + HR * DR, D), (HD * DV + HR * DR) ** -0.5, 0.125),
    }


epsilon = 1e-05
branch_scale = 0.8
masked_score = -1e+30

def normalize(values, gain):
    meansq = lax.optimization_barrier(jnp.mean(values * values, axis=-1, keepdims=True))
    return values * lax.rsqrt(meansq + epsilon) * gain

def rounded(values):
    return lax.optimization_barrier(values.astype(jnp.bfloat16)).astype(jnp.float32)

def differential(att_query, att_keys, att_values, map_lambda, diff_gain):
    length = att_query.shape[0]
    blocks = length // TOK_DEV
    query_float = att_query.reshape(blocks, TOK_DEV, HD, 2, DK).astype(jnp.float32)
    key_float = att_keys.reshape(length, HD, 2, DK).astype(jnp.float32)
    value_float = att_values.reshape(length, HD, DV).astype(jnp.float32)
    key_place = jnp.arange(length)

    def one_block(inputs):
        block_index, query_block = inputs
        query_place = block_index * TOK_DEV + jnp.arange(TOK_DEV)
        scores = jnp.einsum('qhmd,khmd->mhqk', query_block, key_float) * DK ** (-0.5)
        causal = key_place[None, :] <= query_place[:, None]
        row_peak = lax.optimization_barrier(jnp.max(jnp.where(causal, scores, masked_score), axis=-1, keepdims=True))
        weights = jnp.where(causal, jnp.exp(scores - row_peak), 0.0)
        totals = lax.optimization_barrier(jnp.sum(weights, axis=-1, keepdims=True))
        averaged = jnp.einsum('mhqk,khv->mhqv', rounded(weights), value_float) / totals
        differ = averaged[0] - map_lambda[:, None, None] * averaged[1]
        normed = normalize(differ, diff_gain.reshape(HD, 1, DV)) * branch_scale
        return normed.transpose(1, 0, 2).reshape(TOK_DEV, HD * DV).astype(jnp.bfloat16)
    outputs = lax.map(one_block, (jnp.arange(blocks), query_float))
    return outputs.reshape(length, HD * DV)

def retention(ret_query, ret_keys, ret_values, decay_rate, state_gain):
    length = ret_query.shape[0]
    blocks = length // TOK_DEV

    def to_blocks(array):
        return array.reshape(blocks, TOK_DEV, HR, DR)
    position = jnp.arange(TOK_DEV).astype(jnp.float32)
    distance = position[:, None] - position[None, :]
    decay_col = decay_rate[:, None, None]
    within = jnp.where(distance >= 0, jnp.exp(-decay_col * jnp.maximum(distance, 0.0)), 0.0)
    query_decay = jnp.exp(-decay_col * (position + 1.0)[None, :, None])
    key_decay = jnp.exp(-decay_rate[None, :, None] * (TOK_DEV - 1.0 - position)[:, None, None])
    block_decay = jnp.exp(-decay_rate * TOK_DEV)[:, None, None]

    def advance(carry_state, inputs):
        query_block, key_block, value_block = (member.astype(jnp.float32) for member in inputs)
        local_scores = jnp.einsum('qhd,khd->hqk', query_block, key_block) * within
        intra_out = jnp.einsum('hqk,khv->hqv', rounded(local_scores), value_block)
        carried = jnp.einsum('qhd,hdv->hqv', query_block, carry_state, precision=lax.Precision.HIGHEST) * query_decay
        carry_state = carry_state * block_decay + jnp.einsum('khd,khv->hdv', key_block * key_decay, value_block, precision=lax.Precision.HIGHEST)
        normed = normalize(intra_out + carried, state_gain.reshape(HR, 1, DR))
        return (carry_state, normed.transpose(1, 0, 2).reshape(TOK_DEV, HR * DR).astype(jnp.bfloat16))
    initial = jnp.zeros((HR, DR, DR), jnp.float32)
    _, outputs = lax.scan(advance, initial, (to_blocks(ret_query), to_blocks(ret_keys), to_blocks(ret_values)))
    return outputs.reshape(length, HR * DR)

def reference(tokens, norm_gain, query_weight, key_weight, value_weight, state_query, state_key, state_value, map_lambda, diff_gain, decay_rate, state_gain, out_weight):

    def one_sequence(sequence):
        tok_float = sequence.astype(jnp.float32)
        normed = normalize(tok_float, norm_gain).astype(jnp.bfloat16)

        def project(weight):
            return jnp.dot(normed, weight, preferred_element_type=jnp.float32).astype(jnp.bfloat16)
        attended = differential(project(query_weight), project(key_weight), project(value_weight), map_lambda, diff_gain)
        retained = retention(project(state_query), project(state_key), project(state_value), decay_rate, state_gain)
        joined = jnp.concatenate([attended, retained], axis=1)
        return jnp.dot(joined, out_weight, preferred_element_type=jnp.float32).astype(jnp.bfloat16)
    return lax.map(one_sequence, tokens)
```

```python
import jax
import jax.numpy as jnp
from jax import lax
from jax.experimental import pallas as pl
from jax.experimental.pallas import tpu as pltpu
from jax.sharding import PartitionSpec as P

DK = 64
DV = 128
DR = 128


epsilon = 1e-05
branch_scale = 0.8
masked_score = -1e30


def from_behind(x, axis, by):
    size = lax.axis_size(axis)
    pairs = [(i, i + by) for i in range(size) if 0 <= i + by < size]
    return lax.ppermute(x, axis, pairs)


def entering(x, axis, join, neutral):
    place = lax.axis_index(axis)
    gathered = jax.tree.map(
        lambda a, kind: lax.all_gather(a.astype(kind), axis), x, (jnp.bfloat16, jnp.bfloat16)
    )
    state = jax.tree.map(lambda a, e: jnp.zeros_like(a) + jnp.asarray(e, a.dtype), x, neutral)

    def one(turn, state):
        return join(
            state,
            jax.tree.map(
                lambda a, own: lax.dynamic_index_in_dim(a, turn, 0, False).astype(own.dtype),
                gathered,
                x,
            ),
        )

    return lax.fori_loop(0, place, one, state)


def attend(att_query, att_keys, att_values, map_lambda, diff_gain):
    tok_rows = att_query.shape[0]
    head_count = map_lambda.shape[0]
    key_width = att_keys.shape[1]
    query_heads = att_query.reshape(tok_rows, head_count, 2, DK)
    sp_index = lax.axis_index("sp")
    query_place = sp_index * tok_rows + jnp.arange(tok_rows)
    score_scale = DK ** (-0.5)

    def absorb_block(running, inputs):
        key_block, key_place = inputs
        key_heads = key_block[:, :key_width].reshape(tok_rows, head_count, 2, DK)
        value_heads = key_block[:, key_width:].reshape(tok_rows, head_count, DV)
        scores = (
            jnp.einsum(
                "qhmd,khmd->mhqk", query_heads, key_heads, preferred_element_type=jnp.float32
            )
            * score_scale
        )
        causal = key_place[None, :] <= query_place[:, None]
        row_peak, totals, summed = running
        new_peak = jnp.maximum(row_peak, jnp.max(jnp.where(causal, scores, masked_score), axis=-1))
        weights = jnp.where(causal, jnp.exp(scores - new_peak[..., None]), 0.0)
        factor = jnp.exp(row_peak - new_peak)
        totals = totals * factor + jnp.sum(weights, axis=-1)
        summed = summed * factor[..., None] + jnp.einsum(
            "mhqk,khv->mhqv",
            weights.astype(jnp.bfloat16),
            value_heads,
            preferred_element_type=jnp.float32,
        )
        return ((new_peak, totals, summed), None)

    def absorb(running, pieces, first_row):
        piece_rows = pieces.shape[0]
        stacked = pieces.reshape(piece_rows // tok_rows, tok_rows, pieces.shape[1])
        places = (first_row + jnp.arange(piece_rows)).reshape(piece_rows // tok_rows, tok_rows)
        return lax.scan(absorb_block, running, (stacked, places))[0]

    starting = (
        jnp.full((2, head_count, tok_rows), masked_score, jnp.float32),
        jnp.zeros((2, head_count, tok_rows), jnp.float32),
        jnp.zeros((2, head_count, tok_rows, DV), jnp.float32),
    )
    joined_kv = jnp.concatenate([att_keys, att_values], axis=1)
    first_state = absorb(starting, joined_kv, sp_index * tok_rows)

    def relay_step(step_index, relay_state):
        running, moving = relay_state
        moving = from_behind(moving, "sp", 1)
        first_row = (sp_index - step_index) * tok_rows
        running = lax.cond(
            first_row >= 0,
            lambda holding: absorb(holding, moving, first_row),
            lambda holding: holding,
            running,
        )
        return (running, moving)

    running, _ = lax.fori_loop(1, lax.axis_size("sp"), relay_step, (first_state, joined_kv))
    row_peak, totals, summed = running
    averaged = summed / totals[..., None]
    differ = averaged[0] - map_lambda[:, None, None] * averaged[1]
    normed = differ * lax.rsqrt(jnp.mean(differ * differ, axis=-1, keepdims=True) + epsilon)
    normed = normed * diff_gain.reshape(head_count, 1, DV) * branch_scale
    return normed.transpose(1, 0, 2).reshape(tok_rows, head_count * DV).astype(jnp.bfloat16)


def retain(ret_query, ret_keys, ret_values, decay_rate, state_gain):
    tok_rows = ret_query.shape[0]
    head_count = decay_rate.shape[0]
    query_heads = ret_query.reshape(tok_rows, head_count, DR)
    key_heads = ret_keys.reshape(tok_rows, head_count, DR)
    value_heads = ret_values.reshape(tok_rows, head_count, DR)
    position = jnp.arange(tok_rows).astype(jnp.float32)
    distance = position[:, None] - position[None, :]
    decay_col = decay_rate[:, None, None]
    within = jnp.where(distance >= 0, jnp.exp(-decay_col * jnp.maximum(distance, 0.0)), 0.0)
    local_scores = (
        jnp.einsum("qhd,khd->hqk", query_heads, key_heads, preferred_element_type=jnp.float32)
        * within
    )
    intra_out = jnp.einsum(
        "hqk,khv->hqv",
        local_scores.astype(jnp.bfloat16),
        value_heads,
        preferred_element_type=jnp.float32,
    )
    key_decayed = key_heads.astype(jnp.float32) * jnp.exp(
        -decay_rate[None, :, None] * (tok_rows - 1.0 - position)[:, None, None]
    )
    own_state = jnp.einsum(
        "khd,khv->hdv",
        key_decayed,
        value_heads.astype(jnp.float32),
        precision=lax.Precision.HIGHEST,
    )
    block_decay = jnp.exp(-decay_rate * tok_rows)

    def link_states(earlier, later):
        return (earlier[0] * later[1][:, None, None] + later[0], earlier[1] * later[1])

    identity = (jnp.zeros_like(own_state), jnp.ones_like(block_decay))
    incoming, _ = entering((own_state, block_decay), "sp", link_states, identity)
    carried = jnp.einsum(
        "qhd,hdv->hqv", query_heads.astype(jnp.float32), incoming, precision=lax.Precision.HIGHEST
    )
    carried = carried * jnp.exp(-decay_col * (position + 1.0)[None, :, None])
    combined = intra_out + carried
    normed = combined * lax.rsqrt(jnp.mean(combined * combined, axis=-1, keepdims=True) + epsilon)
    normed = normed * state_gain.reshape(head_count, 1, DR)
    return normed.transpose(1, 0, 2).reshape(tok_rows, head_count * DR).astype(jnp.bfloat16)


def body_by_position(
    tokens,
    norm_gain,
    query_weight,
    key_weight,
    value_weight,
    state_query,
    state_key,
    state_value,
    map_lambda,
    diff_gain,
    decay_rate,
    state_gain,
    out_weight,
):
    gathered = lax.all_gather(tokens[0], "tp", axis=1, tiled=True)
    tok_float = gathered.astype(jnp.float32)
    normed = tok_float * lax.rsqrt(
        jnp.mean(tok_float * tok_float, axis=-1, keepdims=True) + epsilon
    )
    normed = (normed * norm_gain).astype(jnp.bfloat16)
    pieces = (
        lax.all_gather(query_weight, "fs", axis=0, tiled=True),
        lax.all_gather(key_weight, "fs", axis=0, tiled=True),
        lax.all_gather(value_weight, "fs", axis=0, tiled=True),
        lax.all_gather(state_query, "fs", axis=0, tiled=True),
        lax.all_gather(state_key, "fs", axis=0, tiled=True),
        lax.all_gather(state_value, "fs", axis=0, tiled=True),
    )
    projected = tuple(
        (jnp.dot(normed, row_block, preferred_element_type=jnp.float32) for row_block in pieces)
    )
    att_query, att_keys, att_values, ret_query, ret_keys, ret_values = (
        member.astype(jnp.bfloat16) for member in projected
    )
    attended = attend(att_query, att_keys, att_values, map_lambda, diff_gain)
    retained = retain(ret_query, ret_keys, ret_values, decay_rate, state_gain)
    joined = jnp.concatenate([attended, retained], axis=1)
    diff_width = attended.shape[1]
    ret_width = retained.shape[1]
    tp_count = lax.axis_size("tp")
    tp_index = lax.axis_index("tp")
    own_rows = jnp.concatenate(
        [
            lax.dynamic_slice_in_dim(out_weight, tp_index * diff_width, diff_width, 0),
            lax.dynamic_slice_in_dim(
                out_weight, tp_count * diff_width + tp_index * ret_width, ret_width, 0
            ),
        ],
        axis=0,
    )
    output = lax.psum_scatter(
        jnp.dot(joined, own_rows, preferred_element_type=jnp.float32).astype(jnp.bfloat16),
        "tp",
        scatter_dimension=0,
        tiled=True,
    )
    return output[None]

def permuted(x, axis, to):
    return lax.ppermute(x, axis, [(i, to(i)) for i in range(lax.axis_size(axis))])


def ring_blocks(x, axis):
    size = lax.axis_size(axis)
    up = lambda i: (i + 1) % size
    down = lambda i: (i - 1) % size
    blocks = {0: [x]}
    ahead, behind = x, x
    for k in range(1, (size - 1) // 2 + 1):
        behind, ahead = permuted(behind, axis, up), permuted(ahead, axis, down)
        blocks[size - k], blocks[k] = [behind], [ahead]
    if size % 2 == 0:
        half = x.shape[0] // 2
        blocks[size // 2] = [
            permuted(behind[:half], axis, up),
            permuted(ahead[half:], axis, down),
        ]
    return [blocks[k] for k in range(size)]


def cube_pieces(w, axis):
    size = lax.axis_size(axis)
    half = w.shape[0] // 2
    send = lambda a, bit: permuted(a, axis, lambda i: i ^ bit)
    whole = {0: w}
    bit = 1
    while bit < size:
        whole[bit] = send(w, bit)
        bit *= 2
    parts = {}

    def part(k, i):
        return whole[k][i * half : (i + 1) * half] if k in whole else parts[k][i]

    for k in range(1, size):
        if k not in whole:
            low = k & -k
            parts[k] = (send(part(k ^ low, 0), low), send(part(low, 1), k ^ low))
    pieces = [(a, k, 0) for k, a in whole.items()]
    for k, pair in parts.items():
        pieces += [(pair[0], k, 0), (pair[1], k, half)]
    return pieces


def call(kernel, outs, scratch, scalars, arrays):
    smem = pl.BlockSpec(memory_space=pltpu.SMEM)
    vmem = pl.BlockSpec(memory_space=pltpu.VMEM)
    return pl.pallas_call(
        kernel,
        out_shape=outs,
        in_specs=[smem] * len(scalars) + [vmem] * len(arrays),
        out_specs=jax.tree.map(lambda _: vmem, outs),
        scratch_shapes=scratch,
    )(*scalars, *arrays)


def normalize_blocks(place, own, other, gain_own, gain_other, rows):
    size = len(own)
    counts = [len(b) for b in own]
    flat = [a for b in own for a in b] + [a for b in other for a in b]
    width = flat[0].shape[1]

    def kernel(place_ref, *refs):
        ins, (go_ref, gs_ref, out_ref) = refs[:-3], refs[-3:]
        half = len(ins) // 2
        n = 0
        for d in range(size):
            start = lax.rem(place_ref[0] + d, size) * rows
            offset = 0
            for _ in range(counts[d]):
                a = ins[n][...].astype(jnp.float32)
                b = ins[half + n][...].astype(jnp.float32)
                total = jnp.sum(a * a, axis=-1, keepdims=True) + jnp.sum(
                    b * b, axis=-1, keepdims=True
                )
                scale = lax.rsqrt(total / (2 * width) + epsilon)
                at = pl.ds(start + offset, a.shape[0])
                out_ref[0, at, :] = (a * scale * go_ref[...]).astype(jnp.bfloat16)
                out_ref[1, at, :] = (b * scale * gs_ref[...]).astype(jnp.bfloat16)
                offset += a.shape[0]
                n += 1

    out = jax.ShapeDtypeStruct((2, size * rows, width), jnp.bfloat16)
    return call(kernel, out, [], [place], flat + [gain_own, gain_other])


def project(place_ref, piece_refs, pieces, normed_ref, weight_ref):
    width = normed_ref.shape[2]
    member_rows = pieces[0][0].shape[0]
    for ref, (_, k, offset) in zip(piece_refs, pieces):
        start = (place_ref[1] ^ k) * member_rows + offset
        weight_ref[pl.ds(start, ref.shape[0]), :] = ref[...]
    own = weight_ref[pl.ds(place_ref[2] * width, width), :]
    other = weight_ref[pl.ds((1 - place_ref[2]) * width, width), :]
    result = jnp.dot(normed_ref[0], own, preferred_element_type=jnp.float32)
    result += jnp.dot(normed_ref[1], other, preferred_element_type=jnp.float32)
    return result.astype(jnp.bfloat16)


def dot_t(a, b):
    return lax.dot_general(a, b, (((1,), (1,)), ((), ())), preferred_element_type=jnp.float32)


def attend_head(place, mix, normed, pieces, gain, rows):
    length = normed.shape[1]
    score_scale = DK ** (-0.5)

    def kernel(place_ref, mix_ref, normed_ref, gain_ref, *refs):
        piece_refs, (out_ref, weight_ref, qkv_ref) = refs[:-3], refs[-3:]
        qkv_ref[...] = project(place_ref, piece_refs, pieces, normed_ref, weight_ref)
        lane = lax.broadcasted_iota(jnp.int32, (rows, 2 * DK), 1)
        below = lax.broadcasted_iota(jnp.int32, (rows, rows), 0) >= lax.broadcasted_iota(
            jnp.int32, (rows, rows), 1
        )
        for block in range(length // rows):
            at = slice(block * rows, (block + 1) * rows)
            query = qkv_ref[at, : 2 * DK]
            outs = []
            for m in range(2):
                mine = (lane >= DK) if m else (lane < DK)
                part = jnp.where(mine, query, jnp.zeros_like(query))
                scores = dot_t(part, qkv_ref[at, 2 * DK : 4 * DK])
                scores = jnp.where(below, scores * score_scale, masked_score)
                peak = jnp.max(scores, axis=-1, keepdims=True)
                if block:
                    past = slice(0, block * rows)
                    before = dot_t(part, qkv_ref[past, 2 * DK : 4 * DK]) * score_scale
                    peak = jnp.maximum(peak, jnp.max(before, axis=-1, keepdims=True))
                weights = jnp.exp(scores - peak)
                total = jnp.sum(weights, axis=-1, keepdims=True)
                summed = jnp.dot(
                    weights.astype(jnp.bfloat16),
                    qkv_ref[at, 4 * DK :],
                    preferred_element_type=jnp.float32,
                )
                if block:
                    weights = jnp.exp(before - peak)
                    total += jnp.sum(weights, axis=-1, keepdims=True)
                    summed += jnp.dot(
                        weights.astype(jnp.bfloat16),
                        qkv_ref[past, 4 * DK :],
                        preferred_element_type=jnp.float32,
                    )
                outs.append(summed / total)
            differ = outs[0] - mix_ref[0] * outs[1]
            scale = lax.rsqrt(jnp.mean(differ * differ, axis=-1, keepdims=True) + epsilon)
            out_ref[at, :] = (differ * scale * gain_ref[...] * branch_scale).astype(jnp.bfloat16)

    columns = pieces[0][0].shape[1]
    height = 2 * normed.shape[2]
    return call(
        kernel,
        jax.ShapeDtypeStruct((length, DV), jnp.bfloat16),
        [pltpu.VMEM((height, columns), jnp.bfloat16), pltpu.VMEM((length, columns), jnp.bfloat16)],
        [place, mix],
        [normed, gain] + [p[0] for p in pieces],
    )


def split_high_low(x):
    high = x.astype(jnp.bfloat16)
    return high, (x - high.astype(jnp.float32)).astype(jnp.bfloat16)


def retain_head(place, rate, normed, pieces, gain, rows):
    length = normed.shape[1]

    def kernel(place_ref, rate_ref, normed_ref, gain_ref, *refs):
        piece_refs, (out_ref, weight_ref, qkv_ref) = refs[:-3], refs[-3:]
        qkv_ref[...] = project(place_ref, piece_refs, pieces, normed_ref, weight_ref)
        r = rate_ref[0]
        distance = lax.broadcasted_iota(jnp.int32, (rows, rows), 0) - lax.broadcasted_iota(
            jnp.int32, (rows, rows), 1
        )
        far = jnp.maximum(distance, 0).astype(jnp.float32)
        within = jnp.where(distance >= 0, jnp.exp(-r * far), 0.0)
        position = lax.broadcasted_iota(jnp.int32, (rows, DR), 0).astype(jnp.float32)
        query_decay = jnp.exp(-r * (position + 1.0))
        key_decay = jnp.exp(-r * (rows - 1.0 - position))
        block_decay = jnp.exp(jnp.full((DR, DR), -r * rows, jnp.float32))
        state = None
        for block in range(length // rows):
            at = slice(block * rows, (block + 1) * rows)
            query = qkv_ref[at, :DR]
            key = qkv_ref[at, DR : 2 * DR]
            value = qkv_ref[at, 2 * DR :]
            local = (dot_t(query, key) * within).astype(jnp.bfloat16)
            total = jnp.dot(local, value, preferred_element_type=jnp.float32)
            if block:
                high, low = split_high_low(state)
                carried = jnp.dot(query, high, preferred_element_type=jnp.float32)
                carried += jnp.dot(query, low, preferred_element_type=jnp.float32)
                total += carried * query_decay
            if (block + 1) * rows < length:
                high, low = split_high_low(key.astype(jnp.float32) * key_decay)
                contract = (((0,), (0,)), ((), ()))
                fresh = lax.dot_general(high, value, contract, preferred_element_type=jnp.float32)
                fresh += lax.dot_general(low, value, contract, preferred_element_type=jnp.float32)
                state = fresh if state is None else state * block_decay + fresh
            scale = lax.rsqrt(jnp.mean(total * total, axis=-1, keepdims=True) + epsilon)
            out_ref[at, :] = (total * scale * gain_ref[...]).astype(jnp.bfloat16)

    columns = pieces[0][0].shape[1]
    height = 2 * normed.shape[2]
    return call(
        kernel,
        jax.ShapeDtypeStruct((length, DR), jnp.bfloat16),
        [pltpu.VMEM((height, columns), jnp.bfloat16), pltpu.VMEM((length, columns), jnp.bfloat16)],
        [place, rate],
        [normed, gain] + [p[0] for p in pieces],
    )


def body_by_head(
    tokens,
    norm_gain,
    query_weight,
    key_weight,
    value_weight,
    state_query,
    state_key,
    state_value,
    map_lambda,
    diff_gain,
    decay_rate,
    state_gain,
    out_weight,
):
    sp_index, fs_index, tp_index = (lax.axis_index(a) for a in ("sp", "fs", "tp"))
    place = jnp.stack([sp_index, fs_index, tp_index]).astype(jnp.int32)
    rows = tokens.shape[1]
    width = tokens.shape[2]

    def head_columns(weight):
        each = weight.shape[-1] // map_lambda.shape[0]
        return lax.dynamic_slice_in_dim(weight, sp_index * each, each, weight.ndim - 1)

    att_own = jnp.concatenate([head_columns(w) for w in (query_weight, key_weight, value_weight)], 1)
    ret_own = jnp.concatenate([head_columns(w) for w in (state_query, state_key, state_value)], 1)
    att_pieces = cube_pieces(att_own, "fs")
    own = ring_blocks(tokens[0], "sp")
    other = [[permuted(a, "tp", lambda i: 1 - i) for a in b] for b in own]
    if lax.axis_size("fs") > 1:
        ret_own, _ = lax.optimization_barrier((ret_own, att_pieces[1][0]))
    ret_pieces = cube_pieces(ret_own, "fs")
    gain_own = lax.dynamic_slice_in_dim(norm_gain, tp_index * width, width)[None]
    gain_other = lax.dynamic_slice_in_dim(norm_gain, (1 - tp_index) * width, width)[None]
    normed = normalize_blocks(place, own, other, gain_own, gain_other, rows)
    attended = attend_head(
        place, head_columns(map_lambda), normed, att_pieces, head_columns(diff_gain)[None], rows
    )
    retained = retain_head(
        place, head_columns(decay_rate), normed, ret_pieces, head_columns(state_gain)[None], rows
    )
    sp_count, tp_count = lax.axis_size("sp"), lax.axis_size("tp")
    joined = jnp.concatenate([attended, retained], axis=1)
    pieces = joined.reshape(sp_count * tp_count, -1, joined.shape[1])
    pieces = lax.all_to_all(pieces, ("sp", "tp"), 0, 0, tiled=True)
    pieces = pieces.reshape(sp_count, tp_count, pieces.shape[1], 2, -1)
    gathered = pieces.transpose(2, 3, 1, 0, 4).reshape(pieces.shape[2], -1)
    output = jnp.dot(gathered, out_weight, preferred_element_type=jnp.float32)
    return output.astype(jnp.bfloat16)[None]


def by_head(mesh, map_lambda, decay_rate):
    size = mesh.shape
    power = size["fs"] & (size["fs"] - 1) == 0
    heads = size["sp"] * size["tp"]
    same = map_lambda.shape[0] == heads and decay_rate.shape[0] == heads
    return power and size["tp"] == 2 and same


def solution(mesh):
    placed = (
        P("fs", "sp", "tp"),
        P(),
        P("fs", "tp"),
        P("fs", "tp"),
        P("fs", "tp"),
        P("fs", "tp"),
        P("fs", "tp"),
        P("fs", "tp"),
        P("tp"),
        P("tp"),
        P("tp"),
        P("tp"),
        P(),
    )

    def run(*arrays):
        body = body_by_head if by_head(mesh, arrays[8], arrays[10]) else body_by_position
        return jax.shard_map(
            body, mesh=mesh, in_specs=placed, out_specs=P("fs", ("sp", "tp"), None), check_vma=False
        )(*arrays)

    return run
```

```python
import jax
import jax.numpy as jnp
from jax import lax
from jax.experimental import pallas as pl
from jax.experimental.pallas import tpu as pltpu
from jax.sharding import PartitionSpec as P

DK = 64
DV = 128
DR = 128


epsilon = 1e-05
branch_scale = 0.8
masked_score = -1e30


def from_behind(x, axis, by):
    size = lax.axis_size(axis)
    pairs = [(i, i + by) for i in range(size) if 0 <= i + by < size]
    return lax.ppermute(x, axis, pairs)


def entering(x, axis, join, neutral):
    place = lax.axis_index(axis)
    gathered = jax.tree.map(
        lambda a, kind: lax.all_gather(a.astype(kind), axis), x, (jnp.bfloat16, jnp.bfloat16)
    )
    state = jax.tree.map(lambda a, e: jnp.zeros_like(a) + jnp.asarray(e, a.dtype), x, neutral)

    def one(turn, state):
        return join(
            state,
            jax.tree.map(
                lambda a, own: lax.dynamic_index_in_dim(a, turn, 0, False).astype(own.dtype),
                gathered,
                x,
            ),
        )

    return lax.fori_loop(0, place, one, state)


def attend(att_query, att_keys, att_values, map_lambda, diff_gain):
    tok_rows = att_query.shape[0]
    head_count = map_lambda.shape[0]
    key_width = att_keys.shape[1]
    query_heads = att_query.reshape(tok_rows, head_count, 2, DK)
    sp_index = lax.axis_index("sp")
    query_place = sp_index * tok_rows + jnp.arange(tok_rows)
    score_scale = DK ** (-0.5)

    def absorb_block(running, inputs):
        key_block, key_place = inputs
        key_heads = key_block[:, :key_width].reshape(tok_rows, head_count, 2, DK)
        value_heads = key_block[:, key_width:].reshape(tok_rows, head_count, DV)
        scores = (
            jnp.einsum(
                "qhmd,khmd->mhqk", query_heads, key_heads, preferred_element_type=jnp.float32
            )
            * score_scale
        )
        causal = key_place[None, :] <= query_place[:, None]
        row_peak, totals, summed = running
        new_peak = jnp.maximum(row_peak, jnp.max(jnp.where(causal, scores, masked_score), axis=-1))
        weights = jnp.where(causal, jnp.exp(scores - new_peak[..., None]), 0.0)
        factor = jnp.exp(row_peak - new_peak)
        totals = totals * factor + jnp.sum(weights, axis=-1)
        summed = summed * factor[..., None] + jnp.einsum(
            "mhqk,khv->mhqv",
            weights.astype(jnp.bfloat16),
            value_heads,
            preferred_element_type=jnp.float32,
        )
        return ((new_peak, totals, summed), None)

    def absorb(running, pieces, first_row):
        piece_rows = pieces.shape[0]
        stacked = pieces.reshape(piece_rows // tok_rows, tok_rows, pieces.shape[1])
        places = (first_row + jnp.arange(piece_rows)).reshape(piece_rows // tok_rows, tok_rows)
        return lax.scan(absorb_block, running, (stacked, places))[0]

    starting = (
        jnp.full((2, head_count, tok_rows), masked_score, jnp.float32),
        jnp.zeros((2, head_count, tok_rows), jnp.float32),
        jnp.zeros((2, head_count, tok_rows, DV), jnp.float32),
    )
    joined_kv = jnp.concatenate([att_keys, att_values], axis=1)
    first_state = absorb(starting, joined_kv, sp_index * tok_rows)

    def relay_step(step_index, relay_state):
        running, moving = relay_state
        moving = from_behind(moving, "sp", 1)
        first_row = (sp_index - step_index) * tok_rows
        running = lax.cond(
            first_row >= 0,
            lambda holding: absorb(holding, moving, first_row),
            lambda holding: holding,
            running,
        )
        return (running, moving)

    running, _ = lax.fori_loop(1, lax.axis_size("sp"), relay_step, (first_state, joined_kv))
    row_peak, totals, summed = running
    averaged = summed / totals[..., None]
    differ = averaged[0] - map_lambda[:, None, None] * averaged[1]
    normed = differ * lax.rsqrt(jnp.mean(differ * differ, axis=-1, keepdims=True) + epsilon)
    normed = normed * diff_gain.reshape(head_count, 1, DV) * branch_scale
    return normed.transpose(1, 0, 2).reshape(tok_rows, head_count * DV).astype(jnp.bfloat16)


def retain(ret_query, ret_keys, ret_values, decay_rate, state_gain):
    tok_rows = ret_query.shape[0]
    head_count = decay_rate.shape[0]
    query_heads = ret_query.reshape(tok_rows, head_count, DR)
    key_heads = ret_keys.reshape(tok_rows, head_count, DR)
    value_heads = ret_values.reshape(tok_rows, head_count, DR)
    position = jnp.arange(tok_rows).astype(jnp.float32)
    distance = position[:, None] - position[None, :]
    decay_col = decay_rate[:, None, None]
    within = jnp.where(distance >= 0, jnp.exp(-decay_col * jnp.maximum(distance, 0.0)), 0.0)
    local_scores = (
        jnp.einsum("qhd,khd->hqk", query_heads, key_heads, preferred_element_type=jnp.float32)
        * within
    )
    intra_out = jnp.einsum(
        "hqk,khv->hqv",
        local_scores.astype(jnp.bfloat16),
        value_heads,
        preferred_element_type=jnp.float32,
    )
    key_decayed = key_heads.astype(jnp.float32) * jnp.exp(
        -decay_rate[None, :, None] * (tok_rows - 1.0 - position)[:, None, None]
    )
    own_state = jnp.einsum(
        "khd,khv->hdv",
        key_decayed,
        value_heads.astype(jnp.float32),
        precision=lax.Precision.HIGHEST,
    )
    block_decay = jnp.exp(-decay_rate * tok_rows)

    def link_states(earlier, later):
        return (earlier[0] * later[1][:, None, None] + later[0], earlier[1] * later[1])

    identity = (jnp.zeros_like(own_state), jnp.ones_like(block_decay))
    incoming, _ = entering((own_state, block_decay), "sp", link_states, identity)
    carried = jnp.einsum(
        "qhd,hdv->hqv", query_heads.astype(jnp.float32), incoming, precision=lax.Precision.HIGHEST
    )
    carried = carried * jnp.exp(-decay_col * (position + 1.0)[None, :, None])
    combined = intra_out + carried
    normed = combined * lax.rsqrt(jnp.mean(combined * combined, axis=-1, keepdims=True) + epsilon)
    normed = normed * state_gain.reshape(head_count, 1, DR)
    return normed.transpose(1, 0, 2).reshape(tok_rows, head_count * DR).astype(jnp.bfloat16)


def body_by_position(
    tokens,
    norm_gain,
    query_weight,
    key_weight,
    value_weight,
    state_query,
    state_key,
    state_value,
    map_lambda,
    diff_gain,
    decay_rate,
    state_gain,
    out_weight,
):
    gathered = lax.all_gather(tokens[0], "tp", axis=1, tiled=True)
    tok_float = gathered.astype(jnp.float32)
    normed = tok_float * lax.rsqrt(
        jnp.mean(tok_float * tok_float, axis=-1, keepdims=True) + epsilon
    )
    normed = (normed * norm_gain).astype(jnp.bfloat16)
    pieces = (
        lax.all_gather(query_weight, "fs", axis=0, tiled=True),
        lax.all_gather(key_weight, "fs", axis=0, tiled=True),
        lax.all_gather(value_weight, "fs", axis=0, tiled=True),
        lax.all_gather(state_query, "fs", axis=0, tiled=True),
        lax.all_gather(state_key, "fs", axis=0, tiled=True),
        lax.all_gather(state_value, "fs", axis=0, tiled=True),
    )
    projected = tuple(
        (jnp.dot(normed, row_block, preferred_element_type=jnp.float32) for row_block in pieces)
    )
    att_query, att_keys, att_values, ret_query, ret_keys, ret_values = (
        member.astype(jnp.bfloat16) for member in projected
    )
    attended = attend(att_query, att_keys, att_values, map_lambda, diff_gain)
    retained = retain(ret_query, ret_keys, ret_values, decay_rate, state_gain)
    joined = jnp.concatenate([attended, retained], axis=1)
    diff_width = attended.shape[1]
    ret_width = retained.shape[1]
    tp_count = lax.axis_size("tp")
    tp_index = lax.axis_index("tp")
    own_rows = jnp.concatenate(
        [
            lax.dynamic_slice_in_dim(out_weight, tp_index * diff_width, diff_width, 0),
            lax.dynamic_slice_in_dim(
                out_weight, tp_count * diff_width + tp_index * ret_width, ret_width, 0
            ),
        ],
        axis=0,
    )
    output = lax.psum_scatter(
        jnp.dot(joined, own_rows, preferred_element_type=jnp.float32).astype(jnp.bfloat16),
        "tp",
        scatter_dimension=0,
        tiled=True,
    )
    return output[None]

def permuted(x, axis, to):
    return lax.ppermute(x, axis, [(i, to(i)) for i in range(lax.axis_size(axis))])


def chain_blocks(x):
    size, pair = lax.axis_size("sp"), lax.axis_size("tp")
    swap = lambda a, valid: lax.ppermute(
        a, ("sp", "tp"), [(s * pair + t, s * pair + 1 - t) for s in valid for t in range(pair)]
    )
    up = down = x
    stages = [[(x, swap(x, range(size)), 0)]]
    for k in range(1, size):
        up = lax.ppermute(up, "sp", [(i, i + 1) for i in range(k - 1, size - 1)])
        down = lax.ppermute(down, "sp", [(i, i - 1) for i in range(1, size - k + 1)])
        stages.append(
            [(up, swap(up, range(k, size)), -k), (down, swap(down, range(size - k)), k)]
        )
    return stages


def cube_pieces(w, axis):
    send = lambda k: permuted(w, axis, lambda i: i ^ k)
    return [(w, 0)] + [(send(k), k) for k in range(1, lax.axis_size(axis))]


def call(kernel, outs, scratch, scalars, arrays):
    smem = pl.BlockSpec(memory_space=pltpu.SMEM)
    vmem = pl.BlockSpec(memory_space=pltpu.VMEM)
    return pl.pallas_call(
        kernel,
        out_shape=outs,
        in_specs=[smem] * len(scalars) + [vmem] * len(arrays),
        out_specs=jax.tree.map(lambda _: vmem, outs),
        scratch_shapes=scratch,
    )(*scalars, *arrays)


def normalize_stage(stage, gain):
    rows, width = stage[0][0].shape
    size = lax.axis_size("sp")
    arrays = [a for own, other, _ in stage for a in (own, other)]

    def kernel(gain_ref, *refs):
        ins, outs = refs[: len(arrays)], refs[len(arrays) :]
        sp_index, tp_index = lax.axis_index("sp"), lax.axis_index("tp")
        for n, (_, _, offset) in enumerate(stage):
            block = sp_index + offset

            @pl.when((block >= 0) & (block < size))
            def _():
                a = ins[2 * n][...].astype(jnp.float32)
                b = ins[2 * n + 1][...].astype(jnp.float32)
                total = jnp.sum(a * a + b * b, axis=-1, keepdims=True)
                scale = lax.rsqrt(total / (2 * width) + epsilon)
                gain_a = gain_ref[pl.ds(tp_index, 1), :]
                gain_b = gain_ref[pl.ds(1 - tp_index, 1), :]
                outs[n][0] = (a * scale * gain_a).astype(jnp.bfloat16)
                outs[n][1] = (b * scale * gain_b).astype(jnp.bfloat16)

    out = [jax.ShapeDtypeStruct((2, rows, width), jnp.bfloat16)] * len(stage)
    normed = call(kernel, out, [], [], [gain.reshape(2, width)] + arrays)
    return [(a, offset) for a, (_, _, offset) in zip(normed, stage)]


def project(normed_refs, offsets, piece_refs, pieces, weight_ref, qkv_ref):
    _, rows, width = normed_refs[0].shape
    member_rows = pieces[0][0].shape[0]
    sp_index, fs_index, tp_index = (lax.axis_index(a) for a in ("sp", "fs", "tp"))
    for ref, (_, k) in zip(piece_refs, pieces):
        weight_ref[pl.ds((fs_index ^ k) * member_rows, member_rows), :] = ref[...]
    for ref, offset in zip(normed_refs, offsets):
        block = sp_index + offset

        @pl.when((block >= 0) & (block * rows < qkv_ref.shape[0]))
        def _():
            own = weight_ref[pl.ds(tp_index * width, width), :]
            other = weight_ref[pl.ds((1 - tp_index) * width, width), :]
            result = jnp.dot(ref[0], own, preferred_element_type=jnp.float32)
            result += jnp.dot(ref[1], other, preferred_element_type=jnp.float32)
            qkv_ref[pl.ds(block * rows, rows), :] = result.astype(jnp.bfloat16)


def mix_head(kernel_of, scalars, gain, normed, pieces):
    _, rows, width = normed[0][0].shape
    size = lax.axis_size("sp")
    columns = pieces[0][0].shape[1]
    head_width = gain.shape[0] // size
    offsets = [offset for _, offset in normed]

    def kernel(scalar_ref, gain_ref, *refs):
        normed_refs, refs = refs[: len(normed)], refs[len(normed) :]
        piece_refs, refs = refs[: len(pieces)], refs[len(pieces) :]
        out_refs, (weight_ref, qkv_ref, mixed_ref) = refs[:size], refs[size:]
        project(normed_refs, offsets, piece_refs, pieces, weight_ref, qkv_ref)
        sp_index = lax.axis_index("sp")

        def store(block, value):
            ahead = lax.rem(block - sp_index + size, size)
            mixed_ref[pl.ds(ahead * rows, rows), :] = value

        kernel_of(scalar_ref[sp_index], gain_ref[pl.ds(sp_index, 1), :], qkv_ref, rows, store)
        for k, ref in enumerate(out_refs):
            ref[...] = mixed_ref[k * rows : (k + 1) * rows, :]

    length = size * rows
    return call(
        kernel,
        [jax.ShapeDtypeStruct((rows, head_width), jnp.bfloat16)] * size,
        [
            pltpu.VMEM((2 * width, columns), jnp.bfloat16),
            pltpu.VMEM((length, columns), jnp.bfloat16),
            pltpu.VMEM((length, head_width), jnp.bfloat16),
        ],
        [scalars],
        [gain.reshape(size, head_width)] + [a for a, _ in normed] + [p[0] for p in pieces],
    )


def exchange_positions(blocks):
    size = lax.axis_size("sp")
    got = [blocks[0]] + [
        permuted(blocks[k], "sp", lambda i: (i + k) % size) for k in range(1, size)
    ]
    return got


def exchange_halves(got):
    tp_index = lax.axis_index("tp")
    joined = jnp.concatenate(got, axis=1)
    half = joined.shape[0] // 2
    mine = lax.dynamic_slice_in_dim(joined, tp_index * half, half, 0)
    theirs = lax.dynamic_slice_in_dim(joined, (1 - tp_index) * half, half, 0)
    return mine, permuted(theirs, "tp", lambda i: 1 - i)


def output_product(pairs, out_weight):
    size = lax.axis_size("sp")
    rows = pairs[0][0].shape[0]
    head_width = pairs[0][0].shape[1] // size

    def kernel(weight_ref, *refs):
        ins, (out_ref, left_ref) = refs[:-2], refs[-2:]
        sp_index, tp_index = lax.axis_index("sp"), lax.axis_index("tp")
        columns = size * head_width
        for n, ref in enumerate(ins):
            side = tp_index if n % 2 == 0 else 1 - tp_index
            for k in range(size):
                head = lax.rem(sp_index - k + size, size)
                at = (n // 2 * 2 + side) * columns + head * head_width
                left_ref[:, pl.ds(pl.multiple_of(at, head_width), head_width)] = ref[
                    :, k * head_width : (k + 1) * head_width
                ]
        out_ref[...] = jnp.dot(
            left_ref[...], weight_ref[...], preferred_element_type=jnp.float32
        ).astype(jnp.bfloat16)

    return call(
        kernel,
        jax.ShapeDtypeStruct((rows, out_weight.shape[1]), jnp.bfloat16),
        [pltpu.VMEM((rows, out_weight.shape[0]), jnp.bfloat16)],
        [],
        [out_weight] + [a for pair in pairs for a in pair],
    )


def dot_t(a, b):
    return lax.dot_general(a, b, (((1,), (1,)), ((), ())), preferred_element_type=jnp.float32)


def attend_head(mix, gain, qkv_ref, rows, store):
    score_scale = DK ** (-0.5)
    lane = lax.broadcasted_iota(jnp.int32, (rows, 2 * DK), 1)
    below = lax.broadcasted_iota(jnp.int32, (rows, rows), 0) >= lax.broadcasted_iota(
        jnp.int32, (rows, rows), 1
    )
    for block in range(qkv_ref.shape[0] // rows):
        at = slice(block * rows, (block + 1) * rows)
        query = qkv_ref[at, : 2 * DK]
        outs = []
        for m in range(2):
            mine = (lane >= DK) if m else (lane < DK)
            part = jnp.where(mine, query, jnp.zeros_like(query))
            scores = dot_t(part, qkv_ref[at, 2 * DK : 4 * DK])
            scores = jnp.where(below, scores * score_scale, masked_score)
            peak = jnp.max(scores, axis=-1, keepdims=True)
            if block:
                past = slice(0, block * rows)
                before = dot_t(part, qkv_ref[past, 2 * DK : 4 * DK]) * score_scale
                peak = jnp.maximum(peak, jnp.max(before, axis=-1, keepdims=True))
            weights = jnp.exp(scores - peak)
            total = jnp.sum(weights, axis=-1, keepdims=True)
            summed = jnp.dot(
                weights.astype(jnp.bfloat16),
                qkv_ref[at, 4 * DK :],
                preferred_element_type=jnp.float32,
            )
            if block:
                weights = jnp.exp(before - peak)
                total += jnp.sum(weights, axis=-1, keepdims=True)
                summed += jnp.dot(
                    weights.astype(jnp.bfloat16),
                    qkv_ref[past, 4 * DK :],
                    preferred_element_type=jnp.float32,
                )
            outs.append(summed / total)
        differ = outs[0] - mix * outs[1]
        scale = lax.rsqrt(jnp.mean(differ * differ, axis=-1, keepdims=True) + epsilon)
        store(block, (differ * scale * gain * branch_scale).astype(jnp.bfloat16))


def split_high_low(x):
    high = x.astype(jnp.bfloat16)
    return high, (x - high.astype(jnp.float32)).astype(jnp.bfloat16)


def retain_head(r, gain, qkv_ref, rows, store):
    length = qkv_ref.shape[0]
    distance = lax.broadcasted_iota(jnp.int32, (rows, rows), 0) - lax.broadcasted_iota(
        jnp.int32, (rows, rows), 1
    )
    far = jnp.maximum(distance, 0).astype(jnp.float32)
    within = jnp.where(distance >= 0, jnp.exp(-r * far), 0.0)
    position = lax.broadcasted_iota(jnp.int32, (rows, DR), 0).astype(jnp.float32)
    query_decay = jnp.exp(-r * (position + 1.0))
    key_decay = jnp.exp(-r * (rows - 1.0 - position))
    block_decay = jnp.exp(jnp.full((DR, DR), -r * rows, jnp.float32))
    state = None
    for block in range(length // rows):
        at = slice(block * rows, (block + 1) * rows)
        query = qkv_ref[at, :DR]
        key = qkv_ref[at, DR : 2 * DR]
        value = qkv_ref[at, 2 * DR :]
        local = (dot_t(query, key) * within).astype(jnp.bfloat16)
        total = jnp.dot(local, value, preferred_element_type=jnp.float32)
        if block:
            high, low = split_high_low(state)
            carried = jnp.dot(query, high, preferred_element_type=jnp.float32)
            carried += jnp.dot(query, low, preferred_element_type=jnp.float32)
            total += carried * query_decay
        if (block + 1) * rows < length:
            high, low = split_high_low(key.astype(jnp.float32) * key_decay)
            contract = (((0,), (0,)), ((), ()))
            fresh = lax.dot_general(high, value, contract, preferred_element_type=jnp.float32)
            fresh += lax.dot_general(low, value, contract, preferred_element_type=jnp.float32)
            state = fresh if state is None else state * block_decay + fresh
        scale = lax.rsqrt(jnp.mean(total * total, axis=-1, keepdims=True) + epsilon)
        store(block, (total * scale * gain).astype(jnp.bfloat16))


def body_by_head(
    tokens,
    norm_gain,
    query_weight,
    key_weight,
    value_weight,
    state_query,
    state_key,
    state_value,
    map_lambda,
    diff_gain,
    decay_rate,
    state_gain,
    out_weight,
):
    sp_index = lax.axis_index("sp")

    def head_columns(*weights):
        each = weights[0].shape[1] // map_lambda.shape[0]
        return jnp.concatenate(
            [lax.dynamic_slice_in_dim(w, sp_index * each, each, 1) for w in weights], axis=1
        )

    att_own = head_columns(query_weight, key_weight, value_weight)
    ret_own = head_columns(state_query, state_key, state_value)
    stages = chain_blocks(tokens[0])
    att_pieces = cube_pieces(att_own, "fs")
    ret_pieces = cube_pieces(ret_own, "fs")
    normed = [block for stage in stages for block in normalize_stage(stage, norm_gain)]
    attended = mix_head(attend_head, map_lambda, diff_gain, normed, att_pieces)
    attended = exchange_positions(attended)
    retained = mix_head(retain_head, decay_rate, state_gain, normed, ret_pieces)
    retained = exchange_positions(retained)
    pairs = [exchange_halves(attended), exchange_halves(retained)]
    return output_product(pairs, out_weight)[None]


def by_head(mesh, map_lambda, decay_rate):
    size = mesh.shape
    power = size["fs"] & (size["fs"] - 1) == 0
    heads = size["sp"] * size["tp"]
    same = map_lambda.shape[0] == heads and decay_rate.shape[0] == heads
    return power and size["tp"] == 2 and same


def solution(mesh):
    placed = (
        P("fs", "sp", "tp"),
        P(),
        P("fs", "tp"),
        P("fs", "tp"),
        P("fs", "tp"),
        P("fs", "tp"),
        P("fs", "tp"),
        P("fs", "tp"),
        P("tp"),
        P("tp"),
        P("tp"),
        P("tp"),
        P(),
    )

    def run(*arrays):
        body = body_by_head if by_head(mesh, arrays[8], arrays[10]) else body_by_position
        return jax.shard_map(
            body, mesh=mesh, in_specs=placed, out_specs=P("fs", ("sp", "tp"), None), check_vma=False
        )(*arrays)

    return run
```

```python
import jax
import jax.numpy as jnp
from jax import lax
from jax.experimental import pallas as pl
from jax.experimental.pallas import tpu as pltpu
from jax.sharding import PartitionSpec as P


DK = 64
DV = 128
DR = 128


epsilon = 1e-05
branch_scale = 0.8
masked_score = -1e30


def from_behind(x, axis, by):
    size = lax.axis_size(axis)
    pairs = [(i, i + by) for i in range(size) if 0 <= i + by < size]
    return lax.ppermute(x, axis, pairs)


def entering(x, axis, join, neutral):
    place = lax.axis_index(axis)
    gathered = jax.tree.map(
        lambda a, kind: lax.all_gather(a.astype(kind), axis), x, (jnp.bfloat16, jnp.bfloat16)
    )
    state = jax.tree.map(lambda a, e: jnp.zeros_like(a) + jnp.asarray(e, a.dtype), x, neutral)

    def one(turn, state):
        return join(
            state,
            jax.tree.map(
                lambda a, own: lax.dynamic_index_in_dim(a, turn, 0, False).astype(own.dtype),
                gathered,
                x,
            ),
        )

    return lax.fori_loop(0, place, one, state)


def attend(att_query, att_keys, att_values, map_lambda, diff_gain):
    tok_rows = att_query.shape[0]
    head_count = map_lambda.shape[0]
    key_width = att_keys.shape[1]
    query_heads = att_query.reshape(tok_rows, head_count, 2, DK)
    sp_index = lax.axis_index("sp")
    query_place = sp_index * tok_rows + jnp.arange(tok_rows)
    score_scale = DK ** (-0.5)

    def absorb_block(running, inputs):
        key_block, key_place = inputs
        key_heads = key_block[:, :key_width].reshape(tok_rows, head_count, 2, DK)
        value_heads = key_block[:, key_width:].reshape(tok_rows, head_count, DV)
        scores = (
            jnp.einsum(
                "qhmd,khmd->mhqk", query_heads, key_heads, preferred_element_type=jnp.float32
            )
            * score_scale
        )
        causal = key_place[None, :] <= query_place[:, None]
        row_peak, totals, summed = running
        new_peak = jnp.maximum(row_peak, jnp.max(jnp.where(causal, scores, masked_score), axis=-1))
        weights = jnp.where(causal, jnp.exp(scores - new_peak[..., None]), 0.0)
        factor = jnp.exp(row_peak - new_peak)
        totals = totals * factor + jnp.sum(weights, axis=-1)
        summed = summed * factor[..., None] + jnp.einsum(
            "mhqk,khv->mhqv",
            weights.astype(jnp.bfloat16),
            value_heads,
            preferred_element_type=jnp.float32,
        )
        return ((new_peak, totals, summed), None)

    def absorb(running, pieces, first_row):
        piece_rows = pieces.shape[0]
        stacked = pieces.reshape(piece_rows // tok_rows, tok_rows, pieces.shape[1])
        places = (first_row + jnp.arange(piece_rows)).reshape(piece_rows // tok_rows, tok_rows)
        return lax.scan(absorb_block, running, (stacked, places))[0]

    starting = (
        jnp.full((2, head_count, tok_rows), masked_score, jnp.float32),
        jnp.zeros((2, head_count, tok_rows), jnp.float32),
        jnp.zeros((2, head_count, tok_rows, DV), jnp.float32),
    )
    joined_kv = jnp.concatenate([att_keys, att_values], axis=1)
    first_state = absorb(starting, joined_kv, sp_index * tok_rows)

    def relay_step(step_index, relay_state):
        running, moving = relay_state
        moving = from_behind(moving, "sp", 1)
        first_row = (sp_index - step_index) * tok_rows
        running = lax.cond(
            first_row >= 0,
            lambda holding: absorb(holding, moving, first_row),
            lambda holding: holding,
            running,
        )
        return (running, moving)

    running, _ = lax.fori_loop(1, lax.axis_size("sp"), relay_step, (first_state, joined_kv))
    _, totals, summed = running
    averaged = summed / totals[..., None]
    differ = averaged[0] - map_lambda[:, None, None] * averaged[1]
    normed = differ * lax.rsqrt(jnp.mean(differ * differ, axis=-1, keepdims=True) + epsilon)
    normed = normed * diff_gain.reshape(head_count, 1, DV) * branch_scale
    return normed.transpose(1, 0, 2).reshape(tok_rows, head_count * DV).astype(jnp.bfloat16)


def retain(ret_query, ret_keys, ret_values, decay_rate, state_gain):
    tok_rows = ret_query.shape[0]
    head_count = decay_rate.shape[0]
    query_heads = ret_query.reshape(tok_rows, head_count, DR)
    key_heads = ret_keys.reshape(tok_rows, head_count, DR)
    value_heads = ret_values.reshape(tok_rows, head_count, DR)
    position = jnp.arange(tok_rows).astype(jnp.float32)
    distance = position[:, None] - position[None, :]
    decay_col = decay_rate[:, None, None]
    within = jnp.where(distance >= 0, jnp.exp(-decay_col * jnp.maximum(distance, 0.0)), 0.0)
    local_scores = (
        jnp.einsum("qhd,khd->hqk", query_heads, key_heads, preferred_element_type=jnp.float32)
        * within
    )
    intra_out = jnp.einsum(
        "hqk,khv->hqv",
        local_scores.astype(jnp.bfloat16),
        value_heads,
        preferred_element_type=jnp.float32,
    )
    key_decayed = key_heads.astype(jnp.float32) * jnp.exp(
        -decay_rate[None, :, None] * (tok_rows - 1.0 - position)[:, None, None]
    )
    own_state = jnp.einsum(
        "khd,khv->hdv",
        key_decayed,
        value_heads.astype(jnp.float32),
        precision=lax.Precision.HIGHEST,
    )
    block_decay = jnp.exp(-decay_rate * tok_rows)

    def link_states(earlier, later):
        return (earlier[0] * later[1][:, None, None] + later[0], earlier[1] * later[1])

    identity = (jnp.zeros_like(own_state), jnp.ones_like(block_decay))
    incoming, _ = entering((own_state, block_decay), "sp", link_states, identity)
    carried = jnp.einsum(
        "qhd,hdv->hqv", query_heads.astype(jnp.float32), incoming, precision=lax.Precision.HIGHEST
    )
    carried = carried * jnp.exp(-decay_col * (position + 1.0)[None, :, None])
    combined = intra_out + carried
    normed = combined * lax.rsqrt(jnp.mean(combined * combined, axis=-1, keepdims=True) + epsilon)
    normed = normed * state_gain.reshape(head_count, 1, DR)
    return normed.transpose(1, 0, 2).reshape(tok_rows, head_count * DR).astype(jnp.bfloat16)


def body_by_position(
    tokens,
    norm_gain,
    query_weight,
    key_weight,
    value_weight,
    state_query,
    state_key,
    state_value,
    map_lambda,
    diff_gain,
    decay_rate,
    state_gain,
    out_weight,
):
    gathered = lax.all_gather(tokens[0], "tp", axis=1, tiled=True)
    tok_float = gathered.astype(jnp.float32)
    normed = tok_float * lax.rsqrt(
        jnp.mean(tok_float * tok_float, axis=-1, keepdims=True) + epsilon
    )
    normed = (normed * norm_gain).astype(jnp.bfloat16)
    pieces = (
        lax.all_gather(query_weight, "fs", axis=0, tiled=True),
        lax.all_gather(key_weight, "fs", axis=0, tiled=True),
        lax.all_gather(value_weight, "fs", axis=0, tiled=True),
        lax.all_gather(state_query, "fs", axis=0, tiled=True),
        lax.all_gather(state_key, "fs", axis=0, tiled=True),
        lax.all_gather(state_value, "fs", axis=0, tiled=True),
    )
    projected = tuple(
        (jnp.dot(normed, row_block, preferred_element_type=jnp.float32) for row_block in pieces)
    )
    att_query, att_keys, att_values, ret_query, ret_keys, ret_values = (
        member.astype(jnp.bfloat16) for member in projected
    )
    attended = attend(att_query, att_keys, att_values, map_lambda, diff_gain)
    retained = retain(ret_query, ret_keys, ret_values, decay_rate, state_gain)
    joined = jnp.concatenate([attended, retained], axis=1)
    diff_width = attended.shape[1]
    ret_width = retained.shape[1]
    tp_count = lax.axis_size("tp")
    tp_index = lax.axis_index("tp")
    own_rows = jnp.concatenate(
        [
            lax.dynamic_slice_in_dim(out_weight, tp_index * diff_width, diff_width, 0),
            lax.dynamic_slice_in_dim(
                out_weight, tp_count * diff_width + tp_index * ret_width, ret_width, 0
            ),
        ],
        axis=0,
    )
    output = lax.psum_scatter(
        jnp.dot(joined, own_rows, preferred_element_type=jnp.float32).astype(jnp.bfloat16),
        "tp",
        scatter_dimension=0,
        tiled=True,
    )
    return output[None]


def permuted(x, axis, to):
    return lax.ppermute(x, axis, [(i, to(i)) for i in range(lax.axis_size(axis))])


def chain_blocks(x):
    size, pair = lax.axis_size("sp"), lax.axis_size("tp")

    def swap(a, valid):
        pairs = [(s * pair + t, s * pair + 1 - t) for s in valid for t in range(pair)]
        return lax.ppermute(a, ("sp", "tp"), pairs)

    up = down = x
    stages = [[(x, swap(x, range(size)), 0)]]
    for k in range(1, size):
        up = lax.ppermute(up, "sp", [(i, i + 1) for i in range(k - 1, size - 1)])
        down = lax.ppermute(down, "sp", [(i, i - 1) for i in range(1, size - k + 1)])
        from_up = (up, swap(up, range(k, size)), -k)
        stages.append([from_up, (down, swap(down, range(size - k)), k)])
    return stages


def cube_pieces(w, axis):
    send = lambda k: permuted(w, axis, lambda i: i ^ k)
    return [(w, 0)] + [(send(k), k) for k in range(1, lax.axis_size(axis))]


def call(kernel, outs, scratch, scalars, arrays):
    smem = pl.BlockSpec(memory_space=pltpu.SMEM)
    vmem = pl.BlockSpec(memory_space=pltpu.VMEM)
    return pl.pallas_call(
        kernel,
        out_shape=outs,
        in_specs=[smem] * len(scalars) + [vmem] * len(arrays),
        out_specs=jax.tree.map(lambda _: vmem, outs),
        scratch_shapes=scratch,
    )(*scalars, *arrays)


def normalize_stage(stage, gain):
    rows, width = stage[0][0].shape
    size = lax.axis_size("sp")
    arrays = [a for own, other, _ in stage for a in (own, other)]

    def kernel(gain_ref, *refs):
        ins, outs = refs[: len(arrays)], refs[len(arrays) :]
        sp_index, tp_index = lax.axis_index("sp"), lax.axis_index("tp")
        for n, (_, _, offset) in enumerate(stage):
            block = sp_index + offset

            @pl.when((block >= 0) & (block < size))
            def _():
                a = ins[2 * n][...].astype(jnp.float32)
                b = ins[2 * n + 1][...].astype(jnp.float32)
                total = jnp.sum(a * a + b * b, axis=-1, keepdims=True)
                scale = lax.rsqrt(total / (2 * width) + epsilon)
                gain_a = gain_ref[pl.ds(tp_index, 1), :]
                gain_b = gain_ref[pl.ds(1 - tp_index, 1), :]
                outs[n][0] = (a * scale * gain_a).astype(jnp.bfloat16)
                outs[n][1] = (b * scale * gain_b).astype(jnp.bfloat16)

    out = [jax.ShapeDtypeStruct((2, rows, width), jnp.bfloat16)] * len(stage)
    normed = call(kernel, out, [], [], [gain.reshape(2, width)] + arrays)
    return [(a, offset) for a, (_, _, offset) in zip(normed, stage)]


def project(normed_refs, offsets, piece_refs, pieces, weight_ref, qkv_ref):
    _, rows, width = normed_refs[0].shape
    member_rows = pieces[0][0].shape[0]
    sp_index, fs_index, tp_index = (lax.axis_index(a) for a in ("sp", "fs", "tp"))
    for ref, (_, k) in zip(piece_refs, pieces):
        weight_ref[pl.ds((fs_index ^ k) * member_rows, member_rows), :] = ref[...]
    for ref, offset in zip(normed_refs, offsets):
        block = sp_index + offset

        @pl.when((block >= 0) & (block * rows < qkv_ref.shape[0]))
        def _():
            own = weight_ref[pl.ds(tp_index * width, width), :]
            other = weight_ref[pl.ds((1 - tp_index) * width, width), :]
            result = jnp.dot(ref[0], own, preferred_element_type=jnp.float32)
            result += jnp.dot(ref[1], other, preferred_element_type=jnp.float32)
            qkv_ref[pl.ds(block * rows, rows), :] = result.astype(jnp.bfloat16)


def mix_head(kernel_of, scalars, gain, normed, pieces):
    _, rows, width = normed[0][0].shape
    size = lax.axis_size("sp")
    columns = pieces[0][0].shape[1]
    head_width = gain.shape[0] // size
    offsets = [offset for _, offset in normed]

    def kernel(scalar_ref, gain_ref, *refs):
        normed_refs, refs = refs[: len(normed)], refs[len(normed) :]
        piece_refs, refs = refs[: len(pieces)], refs[len(pieces) :]
        out_refs, (weight_ref, qkv_ref, mixed_ref) = refs[:size], refs[size:]
        project(normed_refs, offsets, piece_refs, pieces, weight_ref, qkv_ref)
        sp_index = lax.axis_index("sp")

        def store(block, value):
            ahead = lax.rem(block - sp_index + size, size)
            mixed_ref[pl.ds(ahead * rows, rows), :] = value

        kernel_of(scalar_ref[sp_index], gain_ref[pl.ds(sp_index, 1), :], qkv_ref, rows, store)
        for k, ref in enumerate(out_refs):
            ref[...] = mixed_ref[k * rows : (k + 1) * rows, :]

    length = size * rows
    return call(
        kernel,
        [jax.ShapeDtypeStruct((rows, head_width), jnp.bfloat16)] * size,
        [
            pltpu.VMEM((2 * width, columns), jnp.bfloat16),
            pltpu.VMEM((length, columns), jnp.bfloat16),
            pltpu.VMEM((length, head_width), jnp.bfloat16),
        ],
        [scalars],
        [gain.reshape(size, head_width)] + [a for a, _ in normed] + [p[0] for p in pieces],
    )


def exchange_positions(blocks):
    size = lax.axis_size("sp")
    got = [blocks[0]] + [
        permuted(blocks[k], "sp", lambda i: (i + k) % size) for k in range(1, size)
    ]
    return got


def exchange_halves(got):
    rows, width = got[0].shape
    half = rows // 2

    def kernel(*refs):
        ins, (mine_ref, theirs_ref) = refs[:-2], refs[-2:]
        tp_index = lax.axis_index("tp")
        for k, ref in enumerate(ins):
            at = slice(k * width, (k + 1) * width)
            mine_ref[:, at] = ref[pl.ds(tp_index * half, half), :]
            theirs_ref[:, at] = ref[pl.ds((1 - tp_index) * half, half), :]

    out = [jax.ShapeDtypeStruct((half, width * len(got)), got[0].dtype)] * 2
    mine, theirs = call(kernel, out, [], [], got)
    return mine, permuted(theirs, "tp", lambda i: 1 - i)


def output_product(pairs, out_weight):
    size = lax.axis_size("sp")
    rows = pairs[0][0].shape[0]
    head_width = pairs[0][0].shape[1] // size

    def kernel(weight_ref, *refs):
        ins, (out_ref, left_ref) = refs[:-2], refs[-2:]
        sp_index, tp_index = lax.axis_index("sp"), lax.axis_index("tp")
        columns = size * head_width
        for n, ref in enumerate(ins):
            side = tp_index if n % 2 == 0 else 1 - tp_index
            for k in range(size):
                head = lax.rem(sp_index - k + size, size)
                at = (n // 2 * 2 + side) * columns + head * head_width
                left_ref[:, pl.ds(pl.multiple_of(at, head_width), head_width)] = ref[
                    :, k * head_width : (k + 1) * head_width
                ]
        out_ref[...] = jnp.dot(
            left_ref[...], weight_ref[...], preferred_element_type=jnp.float32
        ).astype(jnp.bfloat16)

    return call(
        kernel,
        jax.ShapeDtypeStruct((rows, out_weight.shape[1]), jnp.bfloat16),
        [pltpu.VMEM((rows, out_weight.shape[0]), jnp.bfloat16)],
        [],
        [out_weight] + [a for pair in pairs for a in pair],
    )


def dot_t(a, b):
    return lax.dot_general(a, b, (((1,), (1,)), ((), ())), preferred_element_type=jnp.float32)


def attend_head(mix, gain, qkv_ref, rows, store):
    score_scale = DK ** (-0.5)
    lane = lax.broadcasted_iota(jnp.int32, (rows, 2 * DK), 1)
    below = lax.broadcasted_iota(jnp.int32, (rows, rows), 0) >= lax.broadcasted_iota(
        jnp.int32, (rows, rows), 1
    )
    for block in range(qkv_ref.shape[0] // rows):
        at = slice(block * rows, (block + 1) * rows)
        query = qkv_ref[at, : 2 * DK]
        outs = []
        for m in range(2):
            mine = (lane >= DK) if m else (lane < DK)
            part = jnp.where(mine, query, jnp.zeros_like(query))
            scores = dot_t(part, qkv_ref[at, 2 * DK : 4 * DK])
            scores = jnp.where(below, scores * score_scale, masked_score)
            peak = jnp.max(scores, axis=-1, keepdims=True)
            if block:
                past = slice(0, block * rows)
                before = dot_t(part, qkv_ref[past, 2 * DK : 4 * DK]) * score_scale
                peak = jnp.maximum(peak, jnp.max(before, axis=-1, keepdims=True))
            weights = jnp.exp(scores - peak)
            total = jnp.sum(weights, axis=-1, keepdims=True)
            summed = jnp.dot(
                weights.astype(jnp.bfloat16),
                qkv_ref[at, 4 * DK :],
                preferred_element_type=jnp.float32,
            )
            if block:
                weights = jnp.exp(before - peak)
                total += jnp.sum(weights, axis=-1, keepdims=True)
                summed += jnp.dot(
                    weights.astype(jnp.bfloat16),
                    qkv_ref[past, 4 * DK :],
                    preferred_element_type=jnp.float32,
                )
            outs.append(summed / total)
        differ = outs[0] - mix * outs[1]
        scale = lax.rsqrt(jnp.mean(differ * differ, axis=-1, keepdims=True) + epsilon)
        store(block, (differ * scale * gain * branch_scale).astype(jnp.bfloat16))


def split_high_low(x):
    high = x.astype(jnp.bfloat16)
    return high, (x - high.astype(jnp.float32)).astype(jnp.bfloat16)


def retain_head(r, gain, qkv_ref, rows, store):
    length = qkv_ref.shape[0]
    distance = lax.broadcasted_iota(jnp.int32, (rows, rows), 0) - lax.broadcasted_iota(
        jnp.int32, (rows, rows), 1
    )
    far = jnp.maximum(distance, 0).astype(jnp.float32)
    within = jnp.where(distance >= 0, jnp.exp(-r * far), 0.0)
    position = lax.broadcasted_iota(jnp.int32, (rows, DR), 0).astype(jnp.float32)
    query_decay = jnp.exp(-r * (position + 1.0))
    key_decay = jnp.exp(-r * (rows - 1.0 - position))
    block_decay = jnp.exp(jnp.full((DR, DR), -r * rows, jnp.float32))
    state = None
    for block in range(length // rows):
        at = slice(block * rows, (block + 1) * rows)
        query = qkv_ref[at, :DR]
        key = qkv_ref[at, DR : 2 * DR]
        value = qkv_ref[at, 2 * DR :]
        local = (dot_t(query, key) * within).astype(jnp.bfloat16)
        total = jnp.dot(local, value, preferred_element_type=jnp.float32)
        if block:
            high, low = split_high_low(state)
            carried = jnp.dot(query, high, preferred_element_type=jnp.float32)
            carried += jnp.dot(query, low, preferred_element_type=jnp.float32)
            total += carried * query_decay
        if (block + 1) * rows < length:
            high, low = split_high_low(key.astype(jnp.float32) * key_decay)
            contract = (((0,), (0,)), ((), ()))
            fresh = lax.dot_general(high, value, contract, preferred_element_type=jnp.float32)
            fresh += lax.dot_general(low, value, contract, preferred_element_type=jnp.float32)
            state = fresh if state is None else state * block_decay + fresh
        scale = lax.rsqrt(jnp.mean(total * total, axis=-1, keepdims=True) + epsilon)
        store(block, (total * scale * gain).astype(jnp.bfloat16))


def body_by_head(
    tokens,
    norm_gain,
    query_weight,
    key_weight,
    value_weight,
    state_query,
    state_key,
    state_value,
    map_lambda,
    diff_gain,
    decay_rate,
    state_gain,
    out_weight,
):
    sp_index = lax.axis_index("sp")

    def head_columns(*weights):
        each = weights[0].shape[1] // map_lambda.shape[0]
        return jnp.concatenate(
            [lax.dynamic_slice_in_dim(w, sp_index * each, each, 1) for w in weights], axis=1
        )

    att_own = head_columns(query_weight, key_weight, value_weight)
    ret_own = head_columns(state_query, state_key, state_value)
    stages = chain_blocks(tokens[0])
    att_pieces = cube_pieces(att_own, "fs")
    ret_pieces = cube_pieces(ret_own, "fs")
    normed = []
    for stage in stages:
        normed += normalize_stage(stage, norm_gain)
    attended = mix_head(attend_head, map_lambda, diff_gain, normed, att_pieces)
    attended = exchange_positions(attended)
    retained = mix_head(retain_head, decay_rate, state_gain, normed, ret_pieces)
    retained = exchange_positions(retained)
    pairs = [exchange_halves(attended), exchange_halves(retained)]
    return output_product(pairs, out_weight)[None]


def by_head(mesh, map_lambda, decay_rate):
    size = mesh.shape
    power = size["fs"] & (size["fs"] - 1) == 0
    heads = size["sp"] * size["tp"]
    same = map_lambda.shape[0] == heads and decay_rate.shape[0] == heads
    return power and size["tp"] == 2 and same


def solution(mesh):
    placed = (
        P("fs", "sp", "tp"),
        P(),
        P("fs", "tp"),
        P("fs", "tp"),
        P("fs", "tp"),
        P("fs", "tp"),
        P("fs", "tp"),
        P("fs", "tp"),
        P("tp"),
        P("tp"),
        P("tp"),
        P("tp"),
        P(),
    )

    def run(*arrays):
        split = by_head(mesh, arrays[8], arrays[10])

        def body(*own):
            if not split:
                return body_by_position(*own)
            return body_by_head(*own)

        return jax.shard_map(
            body, mesh=mesh, in_specs=placed, out_specs=P("fs", ("sp", "tp"), None), check_vma=False
        )(*arrays)

    return run
```

```python
import jax
import jax.numpy as jnp
from jax import lax
from jax.experimental import pallas as pl
from jax.experimental.pallas import tpu as pltpu
from jax.sharding import PartitionSpec as P


DK = 64
DV = 128
DR = 128


epsilon = 1e-05
branch_scale = 0.8
masked_score = -1e30


def from_behind(x, axis, by):
    size = lax.axis_size(axis)
    pairs = [(i, i + by) for i in range(size) if 0 <= i + by < size]
    return lax.ppermute(x, axis, pairs)


def entering(x, axis, join, neutral):
    place = lax.axis_index(axis)
    gathered = jax.tree.map(
        lambda a, kind: lax.all_gather(a.astype(kind), axis), x, (jnp.bfloat16, jnp.bfloat16)
    )
    state = jax.tree.map(lambda a, e: jnp.zeros_like(a) + jnp.asarray(e, a.dtype), x, neutral)

    def one(turn, state):
        return join(
            state,
            jax.tree.map(
                lambda a, own: lax.dynamic_index_in_dim(a, turn, 0, False).astype(own.dtype),
                gathered,
                x,
            ),
        )

    return lax.fori_loop(0, place, one, state)


def attend(att_query, att_keys, att_values, map_lambda, diff_gain):
    tok_rows = att_query.shape[0]
    head_count = map_lambda.shape[0]
    key_width = att_keys.shape[1]
    query_heads = att_query.reshape(tok_rows, head_count, 2, DK)
    sp_index = lax.axis_index("sp")
    query_place = sp_index * tok_rows + jnp.arange(tok_rows)
    score_scale = DK ** (-0.5)

    def absorb_block(running, inputs):
        key_block, key_place = inputs
        key_heads = key_block[:, :key_width].reshape(tok_rows, head_count, 2, DK)
        value_heads = key_block[:, key_width:].reshape(tok_rows, head_count, DV)
        scores = (
            jnp.einsum(
                "qhmd,khmd->mhqk", query_heads, key_heads, preferred_element_type=jnp.float32
            )
            * score_scale
        )
        causal = key_place[None, :] <= query_place[:, None]
        row_peak, totals, summed = running
        new_peak = jnp.maximum(row_peak, jnp.max(jnp.where(causal, scores, masked_score), axis=-1))
        weights = jnp.where(causal, jnp.exp(scores - new_peak[..., None]), 0.0)
        factor = jnp.exp(row_peak - new_peak)
        totals = totals * factor + jnp.sum(weights, axis=-1)
        summed = summed * factor[..., None] + jnp.einsum(
            "mhqk,khv->mhqv",
            weights.astype(jnp.bfloat16),
            value_heads,
            preferred_element_type=jnp.float32,
        )
        return ((new_peak, totals, summed), None)

    def absorb(running, pieces, first_row):
        piece_rows = pieces.shape[0]
        stacked = pieces.reshape(piece_rows // tok_rows, tok_rows, pieces.shape[1])
        places = (first_row + jnp.arange(piece_rows)).reshape(piece_rows // tok_rows, tok_rows)
        return lax.scan(absorb_block, running, (stacked, places))[0]

    starting = (
        jnp.full((2, head_count, tok_rows), masked_score, jnp.float32),
        jnp.zeros((2, head_count, tok_rows), jnp.float32),
        jnp.zeros((2, head_count, tok_rows, DV), jnp.float32),
    )
    joined_kv = jnp.concatenate([att_keys, att_values], axis=1)
    first_state = absorb(starting, joined_kv, sp_index * tok_rows)

    def relay_step(step_index, relay_state):
        running, moving = relay_state
        moving = from_behind(moving, "sp", 1)
        first_row = (sp_index - step_index) * tok_rows
        running = lax.cond(
            first_row >= 0,
            lambda holding: absorb(holding, moving, first_row),
            lambda holding: holding,
            running,
        )
        return (running, moving)

    running, _ = lax.fori_loop(1, lax.axis_size("sp"), relay_step, (first_state, joined_kv))
    _, totals, summed = running
    averaged = summed / totals[..., None]
    differ = averaged[0] - map_lambda[:, None, None] * averaged[1]
    normed = differ * lax.rsqrt(jnp.mean(differ * differ, axis=-1, keepdims=True) + epsilon)
    normed = normed * diff_gain.reshape(head_count, 1, DV) * branch_scale
    return normed.transpose(1, 0, 2).reshape(tok_rows, head_count * DV).astype(jnp.bfloat16)


def retain(ret_query, ret_keys, ret_values, decay_rate, state_gain):
    tok_rows = ret_query.shape[0]
    head_count = decay_rate.shape[0]
    query_heads = ret_query.reshape(tok_rows, head_count, DR)
    key_heads = ret_keys.reshape(tok_rows, head_count, DR)
    value_heads = ret_values.reshape(tok_rows, head_count, DR)
    position = jnp.arange(tok_rows).astype(jnp.float32)
    distance = position[:, None] - position[None, :]
    decay_col = decay_rate[:, None, None]
    within = jnp.where(distance >= 0, jnp.exp(-decay_col * jnp.maximum(distance, 0.0)), 0.0)
    local_scores = (
        jnp.einsum("qhd,khd->hqk", query_heads, key_heads, preferred_element_type=jnp.float32)
        * within
    )
    intra_out = jnp.einsum(
        "hqk,khv->hqv",
        local_scores.astype(jnp.bfloat16),
        value_heads,
        preferred_element_type=jnp.float32,
    )
    key_decayed = key_heads.astype(jnp.float32) * jnp.exp(
        -decay_rate[None, :, None] * (tok_rows - 1.0 - position)[:, None, None]
    )
    own_state = jnp.einsum(
        "khd,khv->hdv",
        key_decayed,
        value_heads.astype(jnp.float32),
        precision=lax.Precision.HIGHEST,
    )
    block_decay = jnp.exp(-decay_rate * tok_rows)

    def link_states(earlier, later):
        return (earlier[0] * later[1][:, None, None] + later[0], earlier[1] * later[1])

    identity = (jnp.zeros_like(own_state), jnp.ones_like(block_decay))
    incoming, _ = entering((own_state, block_decay), "sp", link_states, identity)
    carried = jnp.einsum(
        "qhd,hdv->hqv", query_heads.astype(jnp.float32), incoming, precision=lax.Precision.HIGHEST
    )
    carried = carried * jnp.exp(-decay_col * (position + 1.0)[None, :, None])
    combined = intra_out + carried
    normed = combined * lax.rsqrt(jnp.mean(combined * combined, axis=-1, keepdims=True) + epsilon)
    normed = normed * state_gain.reshape(head_count, 1, DR)
    return normed.transpose(1, 0, 2).reshape(tok_rows, head_count * DR).astype(jnp.bfloat16)


def body_by_position(
    tokens,
    norm_gain,
    query_weight,
    key_weight,
    value_weight,
    state_query,
    state_key,
    state_value,
    map_lambda,
    diff_gain,
    decay_rate,
    state_gain,
    out_weight,
):
    gathered = lax.all_gather(tokens[0], "tp", axis=1, tiled=True)
    tok_float = gathered.astype(jnp.float32)
    normed = tok_float * lax.rsqrt(
        jnp.mean(tok_float * tok_float, axis=-1, keepdims=True) + epsilon
    )
    normed = (normed * norm_gain).astype(jnp.bfloat16)
    pieces = (
        lax.all_gather(query_weight, "fs", axis=0, tiled=True),
        lax.all_gather(key_weight, "fs", axis=0, tiled=True),
        lax.all_gather(value_weight, "fs", axis=0, tiled=True),
        lax.all_gather(state_query, "fs", axis=0, tiled=True),
        lax.all_gather(state_key, "fs", axis=0, tiled=True),
        lax.all_gather(state_value, "fs", axis=0, tiled=True),
    )
    projected = tuple(
        (jnp.dot(normed, row_block, preferred_element_type=jnp.float32) for row_block in pieces)
    )
    att_query, att_keys, att_values, ret_query, ret_keys, ret_values = (
        member.astype(jnp.bfloat16) for member in projected
    )
    attended = attend(att_query, att_keys, att_values, map_lambda, diff_gain)
    retained = retain(ret_query, ret_keys, ret_values, decay_rate, state_gain)
    joined = jnp.concatenate([attended, retained], axis=1)
    diff_width = attended.shape[1]
    ret_width = retained.shape[1]
    tp_count = lax.axis_size("tp")
    tp_index = lax.axis_index("tp")
    own_rows = jnp.concatenate(
        [
            lax.dynamic_slice_in_dim(out_weight, tp_index * diff_width, diff_width, 0),
            lax.dynamic_slice_in_dim(
                out_weight, tp_count * diff_width + tp_index * ret_width, ret_width, 0
            ),
        ],
        axis=0,
    )
    output = lax.psum_scatter(
        jnp.dot(joined, own_rows, preferred_element_type=jnp.float32).astype(jnp.bfloat16),
        "tp",
        scatter_dimension=0,
        tiled=True,
    )
    return output[None]


def permuted(x, axis, to):
    return lax.ppermute(x, axis, [(i, to(i)) for i in range(lax.axis_size(axis))])


def ring_blocks(x):
    size = lax.axis_size("sp")

    def pair(a, offset, row):
        return (a, permuted(a, "tp", lambda i: 1 - i), offset, row)

    def send(a, by):
        return permuted(a, "sp", lambda i: (i + by) % size)

    behind = ahead = x
    stages = [[pair(x, 0, 0)]]
    for k in range(1, (size - 1) // 2 + 1):
        behind, ahead = send(behind, 1), send(ahead, -1)
        stages.append([pair(behind, size - k, 0), pair(ahead, k, 0)])
    if size % 2 == 0:
        k, half = size // 2, x.shape[0] // 2
        first, second = send(behind[:half], 1), send(ahead[half:], -1)
        stages.append([pair(first, k, 0), pair(second, k, half)])
    return stages


def cube_pieces(w, axis):
    send = lambda k: permuted(w, axis, lambda i: i ^ k)
    return [(w, 0)] + [(send(k), k) for k in range(1, lax.axis_size(axis))]


def call(kernel, outs, scratch, scalars, arrays):
    smem = pl.BlockSpec(memory_space=pltpu.SMEM)
    vmem = pl.BlockSpec(memory_space=pltpu.VMEM)
    return pl.pallas_call(
        kernel,
        out_shape=outs,
        in_specs=[smem] * len(scalars) + [vmem] * len(arrays),
        out_specs=jax.tree.map(lambda _: vmem, outs),
        scratch_shapes=scratch,
    )(*scalars, *arrays)


def normalize_stage(stage, gain):
    width = stage[0][0].shape[1]
    arrays = [a for piece in stage for a in piece[:2]]

    def kernel(gain_ref, *refs):
        ins, outs = refs[: len(arrays)], refs[len(arrays) :]
        tp_index = lax.axis_index("tp")
        gain_a = gain_ref[pl.ds(tp_index, 1), :]
        gain_b = gain_ref[pl.ds(1 - tp_index, 1), :]
        for n in range(len(stage)):
            a = ins[2 * n][...].astype(jnp.float32)
            b = ins[2 * n + 1][...].astype(jnp.float32)
            total = jnp.sum(a * a + b * b, axis=-1, keepdims=True)
            scale = lax.rsqrt(total / (2 * width) + epsilon)
            outs[n][0] = (a * scale * gain_a).astype(jnp.bfloat16)
            outs[n][1] = (b * scale * gain_b).astype(jnp.bfloat16)

    out = [jax.ShapeDtypeStruct((2, *piece[0].shape), jnp.bfloat16) for piece in stage]
    normed = call(kernel, out, [], [], [gain.reshape(2, width)] + arrays)
    return [(a, *piece[2:]) for a, piece in zip(normed, stage)]


def project(normed_refs, places, rows, piece_refs, pieces, weight_ref, qkv_ref):
    width = normed_refs[0].shape[2]
    member_rows = pieces[0][0].shape[0]
    sp_index, fs_index, tp_index = (lax.axis_index(a) for a in ("sp", "fs", "tp"))
    size = lax.axis_size("sp")
    for ref, (_, k) in zip(piece_refs, pieces):
        weight_ref[pl.ds((fs_index ^ k) * member_rows, member_rows), :] = ref[...]
    own = weight_ref[pl.ds(tp_index * width, width), :]
    other = weight_ref[pl.ds((1 - tp_index) * width, width), :]
    for ref, (offset, row) in zip(normed_refs, places):
        result = jnp.dot(ref[0], own, preferred_element_type=jnp.float32)
        result += jnp.dot(ref[1], other, preferred_element_type=jnp.float32)
        start = lax.rem(sp_index + offset, size) * rows + row
        qkv_ref[pl.ds(start, ref.shape[1]), :] = result.astype(jnp.bfloat16)


def mix_head(kernel_of, scalars, gain, normed, pieces):
    _, rows, width = normed[0][0].shape
    size = lax.axis_size("sp")
    columns = pieces[0][0].shape[1]
    head_width = gain.shape[0] // size
    places = [piece[1:] for piece in normed]

    def kernel(scalar_ref, gain_ref, *refs):
        normed_refs, refs = refs[: len(normed)], refs[len(normed) :]
        piece_refs, refs = refs[: len(pieces)], refs[len(pieces) :]
        out_refs, (weight_ref, qkv_ref, mixed_ref) = refs[:size], refs[size:]
        project(normed_refs, places, rows, piece_refs, pieces, weight_ref, qkv_ref)
        sp_index = lax.axis_index("sp")

        def store(block, value):
            ahead = lax.rem(block - sp_index + size, size)
            mixed_ref[pl.ds(ahead * rows, rows), :] = value

        kernel_of(scalar_ref[sp_index], gain_ref[pl.ds(sp_index, 1), :], qkv_ref, rows, store)
        for k, ref in enumerate(out_refs):
            ref[...] = mixed_ref[k * rows : (k + 1) * rows, :]

    length = size * rows
    return call(
        kernel,
        [jax.ShapeDtypeStruct((rows, head_width), jnp.bfloat16)] * size,
        [
            pltpu.VMEM((2 * width, columns), jnp.bfloat16),
            pltpu.VMEM((length, columns), jnp.bfloat16),
            pltpu.VMEM((length, head_width), jnp.bfloat16),
        ],
        [scalars],
        [gain.reshape(size, head_width)] + [p[0] for p in normed + pieces],
    )


def exchange_positions(blocks):
    size = lax.axis_size("sp")
    got = [blocks[0]] + [
        permuted(blocks[k], "sp", lambda i: (i + k) % size) for k in range(1, size)
    ]
    return got


def exchange_halves(got):
    rows, width = got[0].shape
    half = rows // 2

    def kernel(*refs):
        ins, (mine_ref, theirs_ref) = refs[:-2], refs[-2:]
        tp_index = lax.axis_index("tp")
        for k, ref in enumerate(ins):
            at = slice(k * width, (k + 1) * width)
            mine_ref[:, at] = ref[pl.ds(tp_index * half, half), :]
            theirs_ref[:, at] = ref[pl.ds((1 - tp_index) * half, half), :]

    out = [jax.ShapeDtypeStruct((half, width * len(got)), got[0].dtype)] * 2
    mine, theirs = call(kernel, out, [], [], got)
    return mine, permuted(theirs, "tp", lambda i: 1 - i)


def output_product(pairs, out_weight):
    size = lax.axis_size("sp")
    rows = pairs[0][0].shape[0]
    head_width = pairs[0][0].shape[1] // size

    def kernel(weight_ref, *refs):
        ins, (out_ref, left_ref) = refs[:-2], refs[-2:]
        sp_index, tp_index = lax.axis_index("sp"), lax.axis_index("tp")
        columns = size * head_width
        for n, ref in enumerate(ins):
            side = tp_index if n % 2 == 0 else 1 - tp_index
            for k in range(size):
                head = lax.rem(sp_index - k + size, size)
                at = (n // 2 * 2 + side) * columns + head * head_width
                left_ref[:, pl.ds(pl.multiple_of(at, head_width), head_width)] = ref[
                    :, k * head_width : (k + 1) * head_width
                ]
        out_ref[...] = jnp.dot(
            left_ref[...], weight_ref[...], preferred_element_type=jnp.float32
        ).astype(jnp.bfloat16)

    return call(
        kernel,
        jax.ShapeDtypeStruct((rows, out_weight.shape[1]), jnp.bfloat16),
        [pltpu.VMEM((rows, out_weight.shape[0]), jnp.bfloat16)],
        [],
        [out_weight] + [a for pair in pairs for a in pair],
    )


def dot_t(a, b):
    return lax.dot_general(a, b, (((1,), (1,)), ((), ())), preferred_element_type=jnp.float32)


def attend_head(mix, gain, qkv_ref, rows, store):
    score_scale = DK ** (-0.5)
    lane = lax.broadcasted_iota(jnp.int32, (rows, 2 * DK), 1)
    below = lax.broadcasted_iota(jnp.int32, (rows, rows), 0) >= lax.broadcasted_iota(
        jnp.int32, (rows, rows), 1
    )
    for block in range(qkv_ref.shape[0] // rows):
        at = slice(block * rows, (block + 1) * rows)
        query = qkv_ref[at, : 2 * DK]
        outs = []
        for m in range(2):
            mine = (lane >= DK) if m else (lane < DK)
            part = jnp.where(mine, query, jnp.zeros_like(query))
            scores = dot_t(part, qkv_ref[at, 2 * DK : 4 * DK])
            scores = jnp.where(below, scores * score_scale, masked_score)
            peak = jnp.max(scores, axis=-1, keepdims=True)
            if block:
                past = slice(0, block * rows)
                before = dot_t(part, qkv_ref[past, 2 * DK : 4 * DK]) * score_scale
                peak = jnp.maximum(peak, jnp.max(before, axis=-1, keepdims=True))
            weights = jnp.exp(scores - peak)
            total = jnp.sum(weights, axis=-1, keepdims=True)
            summed = jnp.dot(
                weights.astype(jnp.bfloat16),
                qkv_ref[at, 4 * DK :],
                preferred_element_type=jnp.float32,
            )
            if block:
                weights = jnp.exp(before - peak)
                total += jnp.sum(weights, axis=-1, keepdims=True)
                summed += jnp.dot(
                    weights.astype(jnp.bfloat16),
                    qkv_ref[past, 4 * DK :],
                    preferred_element_type=jnp.float32,
                )
            outs.append(summed / total)
        differ = outs[0] - mix * outs[1]
        scale = lax.rsqrt(jnp.mean(differ * differ, axis=-1, keepdims=True) + epsilon)
        store(block, (differ * scale * gain * branch_scale).astype(jnp.bfloat16))


def split_high_low(x):
    high = x.astype(jnp.bfloat16)
    return high, (x - high.astype(jnp.float32)).astype(jnp.bfloat16)


def retain_head(r, gain, qkv_ref, rows, store):
    length = qkv_ref.shape[0]
    distance = lax.broadcasted_iota(jnp.int32, (rows, rows), 0) - lax.broadcasted_iota(
        jnp.int32, (rows, rows), 1
    )
    far = jnp.maximum(distance, 0).astype(jnp.float32)
    within = jnp.where(distance >= 0, jnp.exp(-r * far), 0.0)
    position = lax.broadcasted_iota(jnp.int32, (rows, DR), 0).astype(jnp.float32)
    query_decay = jnp.exp(-r * (position + 1.0))
    key_decay = jnp.exp(-r * (rows - 1.0 - position))
    block_decay = jnp.exp(jnp.full((DR, DR), -r * rows, jnp.float32))
    state = None
    for block in range(length // rows):
        at = slice(block * rows, (block + 1) * rows)
        query = qkv_ref[at, :DR]
        key = qkv_ref[at, DR : 2 * DR]
        value = qkv_ref[at, 2 * DR :]
        local = (dot_t(query, key) * within).astype(jnp.bfloat16)
        total = jnp.dot(local, value, preferred_element_type=jnp.float32)
        if block:
            high, low = split_high_low(state)
            carried = jnp.dot(query, high, preferred_element_type=jnp.float32)
            carried += jnp.dot(query, low, preferred_element_type=jnp.float32)
            total += carried * query_decay
        if (block + 1) * rows < length:
            high, low = split_high_low(key.astype(jnp.float32) * key_decay)
            contract = (((0,), (0,)), ((), ()))
            fresh = lax.dot_general(high, value, contract, preferred_element_type=jnp.float32)
            fresh += lax.dot_general(low, value, contract, preferred_element_type=jnp.float32)
            state = fresh if state is None else state * block_decay + fresh
        scale = lax.rsqrt(jnp.mean(total * total, axis=-1, keepdims=True) + epsilon)
        store(block, (total * scale * gain).astype(jnp.bfloat16))


def body_by_head(
    tokens,
    norm_gain,
    query_weight,
    key_weight,
    value_weight,
    state_query,
    state_key,
    state_value,
    map_lambda,
    diff_gain,
    decay_rate,
    state_gain,
    out_weight,
):
    sp_index = lax.axis_index("sp")

    def head_columns(*weights):
        each = weights[0].shape[1] // map_lambda.shape[0]
        return jnp.concatenate(
            [lax.dynamic_slice_in_dim(w, sp_index * each, each, 1) for w in weights], axis=1
        )

    att_own = head_columns(query_weight, key_weight, value_weight)
    ret_own = head_columns(state_query, state_key, state_value)
    stages = ring_blocks(tokens[0])
    att_pieces = cube_pieces(att_own, "fs")
    ret_pieces = cube_pieces(ret_own, "fs")
    normed = []
    for stage in stages:
        normed += normalize_stage(stage, norm_gain)
    attended = mix_head(attend_head, map_lambda, diff_gain, normed, att_pieces)
    attended = exchange_positions(attended)
    retained = mix_head(retain_head, decay_rate, state_gain, normed, ret_pieces)
    retained = exchange_positions(retained)
    pairs = [exchange_halves(attended), exchange_halves(retained)]
    return output_product(pairs, out_weight)[None]


def by_head(mesh, map_lambda, decay_rate):
    size = mesh.shape
    power = size["fs"] & (size["fs"] - 1) == 0
    heads = size["sp"] * size["tp"]
    same = map_lambda.shape[0] == heads and decay_rate.shape[0] == heads
    return power and size["tp"] == 2 and same


def solution(mesh):
    placed = (
        P("fs", "sp", "tp"),
        P(),
        P("fs", "tp"),
        P("fs", "tp"),
        P("fs", "tp"),
        P("fs", "tp"),
        P("fs", "tp"),
        P("fs", "tp"),
        P("tp"),
        P("tp"),
        P("tp"),
        P("tp"),
        P(),
    )

    def run(*arrays):
        split = by_head(mesh, arrays[8], arrays[10])

        def body(*own):
            if not split:
                return body_by_position(*own)
            return body_by_head(*own)

        return jax.shard_map(
            body, mesh=mesh, in_specs=placed, out_specs=P("fs", ("sp", "tp"), None), check_vma=False
        )(*arrays)

    return run
```
